32 devices in a mesh: fs: 8 (over z, y), tp: 4 (over x, core).
Axes of the slice: x: 2, y: 2, z: 4, core: 2. Of those that a mesh axis runs over, the one named last changes fastest.
Arguments:
- saved_input: bfloat16 [49152, 2048], P(('fs', 'tp')), may hold values from -6 to 6
- key_cot: bfloat16 [49152, 1024], P(('fs', 'tp')), may hold values from -0.042143017 to 0.042143017
- mixed_out: bfloat16 [49152, 1024], P(('fs', 'tp')), may hold values from -6 to 6
- out_cot: bfloat16 [49152, 2048], P(('fs', 'tp')), may hold values from -0.042143017 to 0.042143017
- key_weight: float32 [2048, 1024], P('fs', 'tp'), may hold values from -0.125 to 0.125
- out_weight: float32 [1024, 2048], P('tp', 'fs'), may hold values from -0.1875 to 0.1875
- bases: bfloat16 [2, 1024, 512], replicated, may hold values from -0.1875 to 0.1875
- first_moment: float32 [2, 2048, 512], P(None, 'fs', 'tp'), may hold values from -64 to 64
- second_moment: float32 [2, 2048, 512], P(None, 'fs', 'tp'), may hold values from 0.25 to 4
Outputs:
- key_weight_new: float32 [2048, 1024], P('fs', 'tp')
- out_weight_new: float32 [1024, 2048], P('tp', 'fs')
- key_step: float32 [2048, 1024], P('fs', 'tp')
- out_step: float32 [1024, 2048], P('tp', 'fs')
- first_new: float32 [2, 2048, 512], P(None, 'fs', 'tp')
- second_new: float32 [2, 2048, 512], P(None, 'fs', 'tp')
- key_copy: bfloat16 [2048, 1024], P(None, 'tp')
- out_copy: bfloat16 [1024, 2048], P('tp')
The draws below stay inside these ranges and needn't reach their ends.
All inputs are finite; a program needn't handle non-finite values.
Results may differ from the reference program's by a relative error of at most 0.0032.
Values may be sent and summed in bfloat16 or wider, within the bound.
A program may use at most 128 MiB of HBM per device.

```python
import math
import jax
import jax.numpy as jnp
from jax import lax

D = 2048
KEY_WIDTH = 1024
RANK = 512
TOK_DEV = 1536
TOKENS = 49152


def scaled_moment(key, rows, cols):
    row_key, col_key, base_key = jax.random.split(key, 3)
    low_end, high_end = (0.3, 3.0)
    row_scale = jnp.exp(jax.random.uniform(row_key, (2, rows, 1), jnp.float32, math.log(low_end), math.log(high_end)))
    col_scale = jnp.exp(jax.random.uniform(col_key, (2, 1, cols), jnp.float32, math.log(low_end), math.log(high_end)))
    normals = jnp.clip(jax.random.normal(base_key, (2, rows, cols), jnp.float32), -4.0, 4.0)
    return normals * row_scale * col_scale


def draw_first_moment(key, part):
    return scaled_moment(jax.random.fold_in(key, 11), D, RANK)


def input_like(key, row_tag, col_tag, width):
    noise = jax.random.normal(jax.random.fold_in(key, col_tag + 1000), (TOKENS, width), jnp.float32)
    return jnp.clip(noise, -6.0, 6.0)


def cotangent_like(key, row_tag, col_tag, width):
    noise = jax.random.normal(jax.random.fold_in(key, col_tag + 1000), (TOKENS, width), jnp.float32)
    spread = float(TOKENS) ** (-0.5)
    column_scale = jnp.exp(jax.random.uniform(jax.random.fold_in(key, col_tag + 2000), (1, width), jnp.float32, math.log(0.5), math.log(2.0)))
    return spread * jnp.clip(noise, -4.0, 4.0) * column_scale


def draw_saved_input(key, part):
    return input_like(key, 101, 201, D).astype(jnp.bfloat16)


def draw_key_cot(key, part):
    return cotangent_like(key, 101, 202, KEY_WIDTH).astype(jnp.bfloat16)


def draw_mixed_out(key, part):
    return input_like(key, 102, 203, KEY_WIDTH).astype(jnp.bfloat16)


def draw_out_cot(key, part):
    return cotangent_like(key, 102, 204, D).astype(jnp.bfloat16)


def levels(key, extent, cuts, smallest, largest):
    loudness = 1.0
    for axis_at, blocks in cuts:
        draws = jax.random.uniform(jax.random.fold_in(jax.random.fold_in(key, 6), axis_at), (blocks,), jnp.float32, smallest / len(cuts), largest / len(cuts))
        loudness = loudness * jnp.repeat(jnp.exp(draws), extent[axis_at] // blocks).reshape((-1,) + (1,) * (len(extent) - 1 - axis_at))
    return loudness


def bell_draw(rng, shape, scale, reach, cuts=(), dtype=jnp.bfloat16):
    drawn = jax.random.normal(rng, shape, jnp.float32) * scale
    if len(cuts) > 0:
        drawn = levels(rng, shape, cuts, -0.22, 0.18) * drawn
    return jnp.clip(drawn, min=-reach, max=reach).astype(dtype)


def setup_inputs(seed: int = 0) -> dict:
    key_of = jax.random.split(jax.random.key(seed), 10)
    saved_input = draw_saved_input(jax.random.fold_in(key_of[9], 71), 0)
    key_cot = draw_key_cot(jax.random.fold_in(key_of[9], 71), 0)
    mixed_out = draw_mixed_out(jax.random.fold_in(key_of[9], 71), 0)
    out_cot = draw_out_cot(jax.random.fold_in(key_of[9], 71), 0)
    key_weight = bell_draw(key_of[4], (D, KEY_WIDTH), D ** -0.5, 0.125, ((0, 8), (1, 4)), jnp.float32)
    out_weight = bell_draw(key_of[5], (KEY_WIDTH, D), KEY_WIDTH ** -0.5, 0.1875, ((0, 4), (1, 8)), jnp.float32)
    bases = bell_draw(key_of[6], (2, KEY_WIDTH, RANK), KEY_WIDTH ** -0.5, 0.1875)
    first_moment = draw_first_moment(jax.random.fold_in(key_of[9], 71), 0)
    second_moment = jnp.clip(jnp.exp(math.log(4.0) - 2.7725887 * jax.random.uniform(key_of[8], (2, D, RANK), jnp.float32) ** levels(key_of[8], (2, D, RANK), ((1, 8), (2, 4)), -0.2, 0.2)), 0.25, 4.0)
    return {"saved_input": saved_input, "key_cot": key_cot, "mixed_out": mixed_out, "out_cot": out_cot, "key_weight": key_weight, "out_weight": out_weight, "bases": bases, "first_moment": first_moment, "second_moment": second_moment}


highest = lax.Precision.HIGHEST
first_decay = 0.8
second_decay = 0.9
learn_rate = 0.01

def reference(saved_input, key_cot, mixed_out, out_cot, key_weight, out_weight, bases, first_moment, second_moment):
    blocks = saved_input.shape[0] // TOK_DEV

    def in_blocks(array):
        return array.reshape(blocks, TOK_DEV, array.shape[1])

    def accumulate(running, pieces):
        inputs_part, key_part, mixed_part, cot_part = pieces
        key_grad = jnp.dot(inputs_part.astype(jnp.float32).T, key_part.astype(jnp.float32), precision=highest)
        out_grad_t = jnp.dot(cot_part.astype(jnp.float32).T, mixed_part.astype(jnp.float32), precision=highest)
        return ((running[0] + key_grad, running[1] + out_grad_t), None)
    empty_sum = jnp.zeros((D, KEY_WIDTH), jnp.float32)
    totals, _ = lax.scan(accumulate, (empty_sum, empty_sum), (in_blocks(saved_input), in_blocks(key_cot), in_blocks(mixed_out), in_blocks(out_cot)))
    gradients = jnp.stack(totals)
    bases_wide = bases.astype(jnp.float32)
    reduced = jnp.einsum('mrk,mkq->mrq', gradients, bases_wide, precision=highest)
    first_new = first_decay * first_moment + (1.0 - first_decay) * reduced
    second_new = second_decay * second_moment + (1.0 - second_decay) * reduced * reduced
    direction = first_new / jnp.sqrt(second_new)
    scales = lax.rsqrt(lax.optimization_barrier(jnp.mean(direction * direction, axis=(1, 2))) + 1.0)
    projected = jnp.einsum('mrq,mkq->mrk', direction, bases_wide, precision=highest)
    scaled = projected * scales[:, None, None]
    key_step = scaled[0]
    out_step = scaled[1].T
    key_new = key_weight - learn_rate * key_step
    out_new = out_weight - learn_rate * out_step
    return (key_new, out_new, key_step, out_step, first_new, second_new, key_new.astype(jnp.bfloat16), out_new.astype(jnp.bfloat16))
```

```python
import functools

import jax
import jax.numpy as jnp
from jax import lax
from jax.experimental import pallas as pl
from jax.experimental.pallas import tpu as pltpu
from jax.sharding import PartitionSpec as P

MESH = pl.DeviceIdType.MESH
f32 = jnp.float32
bf16 = jnp.bfloat16
first_decay = 0.8
second_decay = 0.9
learn_rate = 0.01


def kernel(
    fs, tp,
    x0_hbm, c0_hbm, c1_hbm, x1_hbm,
    key_w, out_w, bases, first_m, second_m,
    key_new, out_new, key_step, out_step, first_new, second_new, key_copy, out_copy,
    x_buf, c_buf, mapped, own, csnd, crcv, s2snd, s2rcv,
    y_own, y_snd, y_rcv, z0_snd, z0_rcv, z1_own, z1_snd, z1_rcv, x1_snd, x1_rcv,
    dirs, ss_snd, ss_rcv, tt_snd, tt_rcv,
    c_in, x_in, c_send, c_recv, s2_send, s2_recv, y_send, y_recv,
    z_send, z_recv, xx_send, xx_recv, d_send, d_recv, sst_send, sst_recv,
    ttt_send, ttt_recv, gz_send, gz_recv, gy_send, gy_recv,
):
    n = tp // 2
    nz = fs // n
    R, Q = first_m.shape[1], first_m.shape[2]
    W = key_w.shape[1]
    T = x_buf.shape[2]
    rank = bases.shape[2]
    half = rank // 2
    rows = n * R
    fi, ti = lax.axis_index("fs"), lax.axis_index("tp")
    core, xi = lax.rem(ti, 2), ti // 2
    zi, yi = fi // n, lax.rem(fi, n)

    def at_x(p):
        return (fi, p * 2 + core)

    def at_y(p):
        return (zi * n + p, ti)

    def at_z(p):
        return (p * n + yi, ti)

    def peer(me, d, size):
        return lax.rem(me + d, size)

    chunk = [peer(zi, 1 + i, nz) for i in range(nz)]
    loads = {}
    for m, (c_hbm, x_hbm) in ((1, (c1_hbm, x1_hbm)), (0, (c0_hbm, x0_hbm))):
        loads["c", m] = pltpu.make_async_copy(c_hbm, c_buf.at[m], c_in.at[m])
        for i in range(nz):
            cols = pl.ds(pl.multiple_of(chunk[i] * rows, 128), rows)
            loads[m, i] = pltpu.make_async_copy(x_hbm.at[:, cols], x_buf.at[m, i], x_in.at[m, i])
    items = [(m, i) for i in range(nz) for m in (1, 0)]
    loads["c", 1].start()
    loads[1, 0].start()
    loads["c", 0].start()
    for item in items[1:]:
        loads[item].start()

    sends = []

    def remote(src, dst, send, recv, where):
        copy = pltpu.make_async_remote_copy(
            src_ref=src, dst_ref=dst, send_sem=send, recv_sem=recv,
            device_id=where, device_id_type=MESH,
        )
        copy.start()
        sends.append(copy)
        return copy

    barrier = pltpu.get_barrier_semaphore()
    for d in range(1, tp):
        pl.semaphore_signal(barrier, inc=1, device_id=(fi, peer(ti, d, tp)), device_id_type=MESH)
    for d in range(1, fs):
        pl.semaphore_signal(barrier, inc=1, device_id=(peer(fi, d, fs), ti), device_id_type=MESH)

    def map_tokens(m):
        tile = T // 3 if T % 3 == 0 else T

        def step(k, carry):
            at = pl.ds(pl.multiple_of(k * tile, 128), tile)
            both = jnp.dot(c_buf[m, at, :], bases[m], preferred_element_type=f32)
            blocks = [both[:, t * Q:(t + 1) * Q] for t in range(tp)]
            pairs = [(blocks[2 * x], blocks[2 * x + 1]) for x in range(n)]
            kept = [jnp.where(core == 0, a, b) for a, b in pairs]
            sent = [jnp.where(core == 0, b, a) for a, b in pairs]
            mapped[m, at, :] = jnp.concatenate(kept + sent, axis=1).astype(bf16)
            return carry

        lax.fori_loop(0, T // tile, step, 0)

    def multiply(m, i):
        loads[m, i].wait()
        part = lax.dot_general(
            x_buf[m, i], mapped[m], (((0,), (0,)), ((), ())), preferred_element_type=f32
        )
        for x in range(n):
            for y in range(n):
                at = (x, y) if m == 0 else (y, x)
                block = part[y * R:(y + 1) * R]
                own[m, i, at[0], at[1]] = block[:, x * Q:(x + 1) * Q]
                csnd[m, i, at[0], at[1]] = block[:, half + x * Q:half + (x + 1) * Q].astype(bf16)

    flows = {}

    def second_stage(m, i):
        flows["c", m, i].wait_recv()
        total = own[m, i] + crcv[m, i].astype(f32)
        own[m, i] = total
        s2snd[m, i] = total.astype(bf16)
        for d in range(1, n):
            p = peer((xi, yi)[m], d, n)
            flows["s2", m, i, d] = remote(
                s2snd.at[m, i, p], s2rcv.at[m, i, d - 1],
                s2_send.at[m, i, d - 1], s2_recv.at[m, i, d - 1], (at_x, at_y)[m](p),
            )

    def third_stage(m, i):
        total = own[m, i, (xi, yi)[m]]
        for d in range(1, n):
            flows["s2", m, i, d].wait_recv()
            total = total + s2rcv[m, i, d - 1].astype(f32)
        if m == 1:
            if i == nz - 1:
                z1_own[...] = total
            else:
                z1_snd[i] = total.astype(bf16)
                flows["z", 1, i] = remote(
                    z1_snd.at[i], z1_rcv.at[i], z_send.at[1, i], z_recv.at[1, i], at_z(chunk[i])
                )
        else:
            y_own[i] = total
            y_snd[i] = total.astype(bf16)
            for d in range(1, n):
                p = peer(yi, d, n)
                flows["y", i, d] = remote(
                    y_snd.at[i, p], y_rcv.at[i, d - 1],
                    y_send.at[i, d - 1], y_recv.at[i, d - 1], at_y(p),
                )

    def fourth_stage(i):
        total = y_own[i, yi]
        for d in range(1, n):
            flows["y", i, d].wait_recv()
            total = total + y_rcv[i, d - 1].astype(f32)
        if i == nz - 1:
            return total
        z0_snd[i] = total.astype(bf16)
        flows["z", 0, i] = remote(
            z0_snd.at[i], z0_rcv.at[i], z_send.at[0, i], z_recv.at[0, i], at_z(chunk[i])
        )

    for k, (m, i) in enumerate(items):
        if i == 0:
            loads["c", m].wait()
            map_tokens(m)
        multiply(m, i)
        if k == 0:
            pl.semaphore_wait(barrier, tp + fs - 2)
        flows["c", m, i] = remote(
            csnd.at[m, i], crcv.at[m, i], c_send.at[m, i], c_recv.at[m, i],
            (fi, xi * 2 + 1 - core),
        )
        if k >= 1:
            second_stage(*items[k - 1])
        if k >= 3:
            third_stage(*items[k - 3])
        if k >= 5 and items[k - 5][0] == 0:
            fourth_stage(items[k - 5][1])
    last = len(items)
    second_stage(*items[last - 1])
    third_stage(*items[last - 3])
    if items[last - 5][0] == 0:
        fourth_stage(items[last - 5][1])
    third_stage(*items[last - 2])
    third_stage(*items[last - 1])
    total0 = None
    for i in range(nz):
        if ("z", 0, i) not in flows:
            total0 = fourth_stage(i)

    total1 = z1_own[...]
    for i in range(nz - 1):
        flows["z", 1, i].wait_recv()
        total1 = total1 + z1_rcv[i].astype(f32)
    z1_own[...] = total1
    x1_snd[...] = total1.astype(bf16)
    for d in range(1, n):
        p = peer(xi, d, n)
        flows["x", d] = remote(
            x1_snd.at[p], x1_rcv.at[d - 1], xx_send.at[d - 1], xx_recv.at[d - 1], at_x(p)
        )

    def update(m, reduced):
        first = first_decay * first_m[m] + (1.0 - first_decay) * reduced
        second = second_decay * second_m[m] + (1.0 - second_decay) * reduced * reduced
        direction = first / jnp.sqrt(second)
        first_new[m] = first
        second_new[m] = second
        dirs[m, ti] = direction.astype(bf16)
        for d in range(1, tp):
            flows["d", m, d] = remote(
                dirs.at[m, ti], dirs.at[m, ti], d_send.at[m, d - 1], d_recv.at[m, d - 1],
                (fi, peer(ti, d, tp)),
            )
        return jnp.sum(direction * direction, keepdims=True)

    for i in range(nz - 1):
        flows["z", 0, i].wait_recv()
        total0 = total0 + z0_rcv[i].astype(f32)
    sum0 = update(0, total0)
    reduced1 = z1_own[xi]
    for d in range(1, n):
        flows["x", d].wait_recv()
        reduced1 = reduced1 + x1_rcv[d - 1].astype(f32)
    sum1 = update(1, reduced1)

    line = lax.broadcasted_iota(jnp.int32, ss_snd.shape, 0)
    squares = jnp.where(line == 0, sum0, sum1)
    ss_snd[...] = squares
    for d in range(1, tp):
        flows["ss", d] = remote(
            ss_snd, ss_rcv.at[d - 1], sst_send.at[d - 1], sst_recv.at[d - 1],
            (fi, peer(ti, d, tp)),
        )
    for d in range(1, tp):
        flows["ss", d].wait_recv()
        squares = squares + ss_rcv[d - 1]
    tt_snd[...] = squares
    for d in range(1, fs):
        flows["tt", d] = remote(
            tt_snd, tt_rcv.at[d - 1], ttt_send.at[d - 1], ttt_recv.at[d - 1],
            (peer(fi, d, fs), ti),
        )
    local = pl.ds(pl.multiple_of(ti * W, 128), W)
    projected = []
    for m in range(2):
        for d in range(1, tp):
            flows["d", m, d].wait_recv()
        whole = jnp.concatenate([dirs[m, t] for t in range(tp)], axis=1)
        base = bases[m, local, :]
        left, right = ((whole, base), (base, whole))[m]
        projected.append(
            lax.dot_general(left, right, (((1,), (1,)), ((), ())), preferred_element_type=f32)
        )
    for d in range(1, fs):
        flows["tt", d].wait_recv()
        squares = squares + tt_rcv[d - 1]
    scales = lax.rsqrt(squares / (fs * R * rank) + 1.0)

    def key_at(f):
        return key_copy.at[pl.ds(pl.multiple_of(f * R, 128), R), :]

    def out_at(f):
        return out_copy.at[:, pl.ds(pl.multiple_of(f * R, 128), R)]

    pieces = (key_at, out_at)

    def to_y(slot, f, m):
        for d in range(1, n):
            flows["gy", slot, d, m] = remote(
                pieces[m](f), pieces[m](f), gy_send.at[slot, d - 1, m], gy_recv.at[slot, d - 1, m],
                at_y(peer(yi, d, n)),
            )

    for m, (step_ref, new_ref, weight) in enumerate(
        ((key_step, key_new, key_w), (out_step, out_new, out_w))
    ):
        step = projected[m] * scales[m:m + 1, 0:1]
        new = weight[...] - learn_rate * step
        step_ref[...] = step
        new_ref[...] = new
        pieces[m](fi)[...] = new.astype(bf16)
        to_y(nz - 1, fi, m)
        for d in range(1, nz):
            flows["gz", d, m] = remote(
                pieces[m](fi), pieces[m](fi), gz_send.at[d - 1, m], gz_recv.at[d - 1, m],
                at_z(peer(zi, d, nz)),
            )
    for d in range(1, nz):
        for m in range(2):
            flows["gz", d, m].wait_recv()
            to_y(d - 1, peer(zi, nz - d, nz) * n + yi, m)
    for slot in range(nz):
        for d in range(1, n):
            for m in range(2):
                flows["gy", slot, d, m].wait_recv()
    for copy in sends:
        copy.wait_send()


def solution(mesh):
    fs, tp = mesh.shape["fs"], mesh.shape["tp"]
    n = tp // 2
    nz = fs // n

    def body(saved_input, key_cot, mixed_out, out_cot, key_weight, out_weight, bases, first_moment, second_moment):
        R, Q = first_moment.shape[1:]
        T, D = saved_input.shape
        K = key_cot.shape[1]
        rank = bases.shape[2]
        rows = n * R
        vmem = pl.BlockSpec(memory_space=pltpu.VMEM)
        hbm = pl.BlockSpec(memory_space=pltpu.HBM)
        dma = pltpu.SemaphoreType.DMA

        def shape(a):
            return jax.ShapeDtypeStruct(a.shape, f32)

        W = key_weight.shape[1]
        outs = (
            shape(key_weight), shape(out_weight), shape(key_weight), shape(out_weight),
            shape(first_moment), shape(second_moment),
            jax.ShapeDtypeStruct((D, W), bf16), jax.ShapeDtypeStruct((W, D), bf16),
        )
        V = pltpu.VMEM
        o = max(n - 1, 1)
        scratch = [
            V((2, nz, T, rows), bf16), V((2, T, K), bf16), V((2, T, rank), bf16),
            V((2, nz, n, n, R, Q), f32), V((2, nz, n, n, R, Q), bf16), V((2, nz, n, n, R, Q), bf16),
            V((2, nz, n, n, R, Q), bf16), V((2, nz, o, n, R, Q), bf16),
            V((nz, n, R, Q), f32), V((nz, n, R, Q), bf16), V((nz, o, R, Q), bf16),
            V((nz - 1, R, Q), bf16), V((nz - 1, R, Q), bf16),
            V((n, R, Q), f32), V((nz - 1, n, R, Q), bf16), V((nz - 1, n, R, Q), bf16),
            V((n, R, Q), bf16), V((o, R, Q), bf16),
            V((2, tp, R, Q), bf16),
            V((8, 128), f32), V((tp - 1, 8, 128), f32), V((8, 128), f32), V((fs - 1, 8, 128), f32),
            dma((2,)), dma((2, nz)), dma((2, nz)), dma((2, nz)),
            dma((2, nz, o)), dma((2, nz, o)), dma((nz, o)), dma((nz, o)),
            dma((2, nz - 1)), dma((2, nz - 1)), dma((o,)), dma((o,)),
            dma((2, tp - 1)), dma((2, tp - 1)), dma((tp - 1,)), dma((tp - 1,)),
            dma((fs - 1,)), dma((fs - 1,)), dma((nz - 1, 2)), dma((nz - 1, 2)),
            dma((nz, o, 2)), dma((nz, o, 2)),
        ]
        return pl.pallas_call(
            functools.partial(kernel, fs, tp),
            out_shape=outs,
            in_specs=[hbm] * 4 + [vmem] * 5,
            out_specs=[vmem] * 8,
            scratch_shapes=scratch,
            compiler_params=pltpu.CompilerParams(
                collective_id=0, has_side_effects=True, vmem_limit_bytes=60 * 1024 * 1024
            ),
        )(saved_input, key_cot, mixed_out, out_cot, key_weight, out_weight, bases, first_moment, second_moment)

    rows_placed = P(("fs", "tp"), None)
    return jax.shard_map(
        body,
        mesh=mesh,
        in_specs=(rows_placed,) * 4
        + (P("fs", "tp"), P("tp", "fs"), P(), P(None, "fs", "tp"), P(None, "fs", "tp")),
        out_specs=(
            P("fs", "tp"), P("tp", "fs"), P("fs", "tp"), P("tp", "fs"),
            P(None, "fs", "tp"), P(None, "fs", "tp"), P(None, "tp"), P("tp", None),
        ),
        check_vma=False,
    )
```

```python
import functools

import jax
import jax.numpy as jnp
from jax import lax
from jax.experimental import pallas as pl
from jax.experimental.pallas import tpu as pltpu
from jax.sharding import PartitionSpec as P

MESH = pl.DeviceIdType.MESH
f32 = jnp.float32
bf16 = jnp.bfloat16
first_decay = 0.8
second_decay = 0.9
learn_rate = 0.01


def kernel(
    fs, tp,
    x0_hbm, c0_hbm, c1_hbm, x1_hbm,
    key_w_hbm, out_w_hbm, bases_hbm, first_hbm, second_hbm,
    key_new, out_new, key_step, out_step, first_new, second_new, key_copy, out_copy,
    key_w, out_w, bases, first_m, second_m, x_buf, c_buf, mapped, own, csnd, crcv, s2snd, s2rcv,
    y_own, y_snd, y_rcv, z0_snd, z0_rcv, z1_own, z1_snd, z1_rcv, x1_snd, x1_rcv,
    dirs, ss_snd, ss_rcv, tt_snd, tt_rcv,
    b_in, w_in, c_in, x_in, c_send, c_recv, s2_send, s2_recv, y_send, y_recv,
    z_send, z_recv, xx_send, xx_recv, d_send, d_recv, sst_send, sst_recv,
    ttt_send, ttt_recv, gz_send, gz_recv, gy_send, gy_recv,
):
    n = tp // 2
    nz = fs // n
    R, Q = first_m.shape[1], first_m.shape[2]
    W = key_w.shape[1]
    T = x_buf.shape[2]
    rank = bases.shape[2]
    half = rank // 2
    rows = n * R
    fi, ti = lax.axis_index("fs"), lax.axis_index("tp")
    core, xi = lax.rem(ti, 2), ti // 2
    zi, yi = fi // n, lax.rem(fi, n)

    def at_x(p):
        return (fi, p * 2 + core)

    def at_y(p):
        return (zi * n + p, ti)

    def at_z(p):
        return (p * n + yi, ti)

    def peer(me, d, size):
        return lax.rem(me + d, size)

    chunk = [peer(zi, 1 + i, nz) for i in range(nz)]
    tiles = 3 if T % 3 == 0 else 1
    tile = T // tiles
    loads = {}
    for m, (c_hbm, x_hbm) in ((1, (c1_hbm, x1_hbm)), (0, (c0_hbm, x0_hbm))):
        loads["b", m] = pltpu.make_async_copy(bases_hbm.at[m], bases.at[m], b_in.at[m])
        for k in range(tiles):
            at = pl.ds(k * tile, tile)
            loads["c", m, k] = pltpu.make_async_copy(c_hbm.at[at], c_buf.at[m, at], c_in.at[m, k])
        for i in range(nz):
            cols = pl.ds(pl.multiple_of(chunk[i] * rows, 128), rows)
            loads[m, i] = pltpu.make_async_copy(x_hbm.at[:, cols], x_buf.at[m, i], x_in.at[m, i])
    rest = (
        (first_hbm, first_m), (second_hbm, second_m), (key_w_hbm, key_w), (out_w_hbm, out_w)
    )
    for k, (source, target) in enumerate(rest):
        loads["w", k] = pltpu.make_async_copy(source, target, w_in.at[k])
    items = [(m, i) for m in (1, 0) for i in range(nz)]
    for copy in loads.values():
        copy.start()

    sends = []

    def remote(src, dst, send, recv, where):
        copy = pltpu.make_async_remote_copy(
            src_ref=src, dst_ref=dst, send_sem=send, recv_sem=recv,
            device_id=where, device_id_type=MESH,
        )
        copy.start()
        sends.append(copy)
        return copy

    barrier = pltpu.get_barrier_semaphore()
    for d in range(1, tp):
        pl.semaphore_signal(barrier, inc=1, device_id=(fi, peer(ti, d, tp)), device_id_type=MESH)
    for d in range(1, fs):
        pl.semaphore_signal(barrier, inc=1, device_id=(peer(fi, d, fs), ti), device_id_type=MESH)

    def map_tokens(m):
        loads["b", m].wait()
        for k in range(tiles):
            loads["c", m, k].wait()
            at = pl.ds(k * tile, tile)
            both = jnp.dot(c_buf[m, at, :], bases[m], preferred_element_type=f32)
            blocks = [both[:, t * Q:(t + 1) * Q] for t in range(tp)]
            pairs = [(blocks[2 * x], blocks[2 * x + 1]) for x in range(n)]
            kept = [jnp.where(core == 0, a, b) for a, b in pairs]
            sent = [jnp.where(core == 0, b, a) for a, b in pairs]
            mapped[m, at, :] = jnp.concatenate(kept + sent, axis=1).astype(bf16)

    def multiply(m, i):
        loads[m, i].wait()
        part = lax.dot_general(
            x_buf[m, i], mapped[m], (((0,), (0,)), ((), ())), preferred_element_type=f32
        )
        for x in range(n):
            for y in range(n):
                at = (x, y) if m == 0 else (y, x)
                block = part[y * R:(y + 1) * R]
                own[m, i, at[0], at[1]] = block[:, x * Q:(x + 1) * Q]
                csnd[m, i, at[0], at[1]] = block[:, half + x * Q:half + (x + 1) * Q].astype(bf16)

    flows = {}

    def second_stage(m, i):
        flows["c", m, i].wait_recv()
        total = own[m, i] + crcv[m, i].astype(f32)
        own[m, i] = total
        s2snd[m, i] = total.astype(bf16)
        for d in range(1, n):
            p = peer((xi, yi)[m], d, n)
            flows["s2", m, i, d] = remote(
                s2snd.at[m, i, p], s2rcv.at[m, i, d - 1],
                s2_send.at[m, i, d - 1], s2_recv.at[m, i, d - 1], (at_x, at_y)[m](p),
            )

    def third_stage(m, i):
        total = own[m, i, (xi, yi)[m]]
        for d in range(1, n):
            flows["s2", m, i, d].wait_recv()
            total = total + s2rcv[m, i, d - 1].astype(f32)
        if m == 1:
            if i == nz - 1:
                z1_own[...] = total
            else:
                z1_snd[i] = total.astype(bf16)
                flows["z", 1, i] = remote(
                    z1_snd.at[i], z1_rcv.at[i], z_send.at[1, i], z_recv.at[1, i], at_z(chunk[i])
                )
        else:
            y_own[i] = total
            y_snd[i] = total.astype(bf16)
            for d in range(1, n):
                p = peer(yi, d, n)
                flows["y", i, d] = remote(
                    y_snd.at[i, p], y_rcv.at[i, d - 1],
                    y_send.at[i, d - 1], y_recv.at[i, d - 1], at_y(p),
                )

    def fourth_stage(i):
        total = y_own[i, yi]
        for d in range(1, n):
            flows["y", i, d].wait_recv()
            total = total + y_rcv[i, d - 1].astype(f32)
        if i == nz - 1:
            return total
        z0_snd[i] = total.astype(bf16)
        flows["z", 0, i] = remote(
            z0_snd.at[i], z0_rcv.at[i], z_send.at[0, i], z_recv.at[0, i], at_z(chunk[i])
        )

    def sum_z1():
        total = z1_own[...]
        for i in range(nz - 1):
            flows["z", 1, i].wait_recv()
            total = total + z1_rcv[i].astype(f32)
        z1_own[...] = total
        x1_snd[...] = total.astype(bf16)
        for d in range(1, n):
            p = peer(xi, d, n)
            flows["x", d] = remote(
                x1_snd.at[p], x1_rcv.at[d - 1], xx_send.at[d - 1], xx_recv.at[d - 1], at_x(p)
            )

    def sum_x1():
        total = z1_own[xi]
        for d in range(1, n):
            flows["x", d].wait_recv()
            total = total + x1_rcv[d - 1].astype(f32)
        return total

    def sum_z0(total):
        for i in range(nz - 1):
            flows["z", 0, i].wait_recv()
            total = total + z0_rcv[i].astype(f32)
        return total

    def update(m, reduced):
        first = first_decay * first_m[m] + (1.0 - first_decay) * reduced
        second = second_decay * second_m[m] + (1.0 - second_decay) * reduced * reduced
        direction = first / jnp.sqrt(second)
        squares = jnp.broadcast_to(jnp.sum(direction * direction, keepdims=True), (8, 128))
        ss_snd[m] = squares
        dirs[m, ti] = direction.astype(bf16)
        for d in range(1, tp):
            where = (fi, peer(ti, d, tp))
            flows["ss", m, d] = remote(
                ss_snd.at[m], ss_rcv.at[m, d - 1], sst_send.at[m, d - 1], sst_recv.at[m, d - 1], where
            )
            flows["d", m, d] = remote(
                dirs.at[m, ti], dirs.at[m, ti], d_send.at[m, d - 1], d_recv.at[m, d - 1], where
            )
        first_new[m] = first
        second_new[m] = second

    def sum_tp(m):
        squares = ss_snd[m]
        for d in range(1, tp):
            flows["ss", m, d].wait_recv()
            squares = squares + ss_rcv[m, d - 1]
        tt_snd[m] = squares
        for d in range(1, fs):
            flows["tt", m, d] = remote(
                tt_snd.at[m], tt_rcv.at[m, d - 1], ttt_send.at[m, d - 1], ttt_recv.at[m, d - 1],
                (peer(fi, d, fs), ti),
            )

    def project(m):
        for d in range(1, tp):
            flows["d", m, d].wait_recv()
        whole = jnp.concatenate([dirs[m, t] for t in range(tp)], axis=1)
        base = bases[m, pl.ds(pl.multiple_of(ti * W, 128), W), :]
        left, right = ((whole, base), (base, whole))[m]
        (key_step, out_step)[m][...] = lax.dot_general(
            left, right, (((1,), (1,)), ((), ())), preferred_element_type=f32
        )

    def key_at(z, y):
        return key_copy.at[pl.ds(pl.multiple_of((z * n + y) * R, 128), R), :]

    def out_at(z, y):
        return out_copy.at[:, pl.ds(pl.multiple_of((z * n + y) * R, 128), R)]

    pieces = (key_at, out_at)

    def line_copy(m, up, hop):
        piece = pieces[m](zi - hop if up else zi + hop, yi)
        side = 0 if up else 1
        return pltpu.make_async_remote_copy(
            src_ref=piece, dst_ref=piece, send_sem=gz_send.at[m, side, hop], recv_sem=gz_recv.at[m, side, hop],
            device_id=at_z(zi + 1 if up else zi - 1), device_id_type=MESH,
        )

    def may_send(up, hop):
        if up:
            return (zi >= hop) & (zi < nz - 1)
        return (zi + hop < nz) & (zi > 0)

    def side_copies(m, z):
        piece = pieces[m](z, yi)
        return [
            pltpu.make_async_remote_copy(
                src_ref=piece, dst_ref=piece, send_sem=gy_send.at[m, z, d - 1], recv_sem=gy_recv.at[m, z, d - 1],
                device_id=at_y(peer(yi, d, n)), device_id_type=MESH,
            )
            for d in range(1, n)
        ]

    def start_line(m, up, hop):
        @pl.when(may_send(up, hop))
        def _():
            line_copy(m, up, hop).start()

    def finish(m):
        squares = tt_snd[m]
        for d in range(1, fs):
            flows["tt", m, d].wait_recv()
            squares = squares + tt_rcv[m, d - 1]
        scale = lax.rsqrt(squares / (fs * R * rank) + 1.0)[0:1, 0:1]
        step_ref, new_ref, weight = ((key_step, key_new, key_w), (out_step, out_new, out_w))[m]
        step = step_ref[...] * scale
        new = weight[...] - learn_rate * step
        pieces[m](zi, yi)[...] = new.astype(bf16)
        for up in (True, False):
            start_line(m, up, 0)
        for copy in side_copies(m, zi):
            copy.start()
        step_ref[...] = step
        new_ref[...] = new

    def relay(m, hop):
        for up in (True, False):
            @pl.when((zi >= hop) if up else (zi + hop < nz))
            def _():
                line_copy(m, up, hop - 1).wait_recv()
                if hop < nz - 1:
                    start_line(m, up, hop)
                for copy in side_copies(m, zi - hop if up else zi + hop):
                    copy.start()

    def close(m):
        for z in range(nz):
            for copy in side_copies(m, z):
                copy.wait_recv()
        for z in range(nz):
            for copy in side_copies(m, z):
                copy.wait_send()
        for hop in range(nz - 1):
            for up in (True, False):
                @pl.when(may_send(up, hop))
                def _():
                    line_copy(m, up, hop).wait_send()

    for k, (m, i) in enumerate(items):
        if i == 0:
            map_tokens(m)
        multiply(m, i)
        if k == 0:
            pl.semaphore_wait(barrier, tp + fs - 2)
        flows["c", m, i] = remote(
            csnd.at[m, i], crcv.at[m, i], c_send.at[m, i], c_recv.at[m, i],
            (fi, xi * 2 + 1 - core),
        )
        if k >= 1:
            second_stage(*items[k - 1])
        if k >= 3:
            third_stage(*items[k - 3])
    second_stage(0, nz - 1)
    for k in range(len(rest)):
        loads["w", k].wait()
    for k in range(len(items) - 3, len(items)):
        if items[k][0] == 1:
            third_stage(*items[k])
    waiting = [items[k][1] for k in range(len(items) - 3, len(items)) if items[k][0] == 0]
    third_stage(0, waiting[0])
    sum_z1()
    for i in waiting[1:]:
        third_stage(0, i)
    for i in range(nz - 2):
        fourth_stage(i)
    update(1, sum_x1())
    fourth_stage(nz - 2)
    total0 = fourth_stage(nz - 1)
    sum_tp(1)
    project(1)
    update(0, sum_z0(total0))
    finish(1)
    sum_tp(0)
    relay(1, 1)
    project(0)
    finish(0)
    for hop in range(2, nz):
        relay(1, hop)
        relay(0, hop - 1)
    relay(0, nz - 1)
    close(1)
    close(0)
    for copy in sends:
        copy.wait_send()


def move_out(*refs):
    count = len(refs) // 2
    copies = [
        pltpu.make_async_copy(refs[k], refs[count + k], refs[-1].at[k]) for k in range(count)
    ]
    for copy in copies:
        copy.start()
    for copy in copies:
        copy.wait()


def solution(mesh):
    fs, tp = mesh.shape["fs"], mesh.shape["tp"]
    n = tp // 2
    nz = fs // n

    def body(saved_input, key_cot, mixed_out, out_cot, key_weight, out_weight, bases, first_moment, second_moment):
        R, Q = first_moment.shape[1:]
        T, D = saved_input.shape
        K = key_cot.shape[1]
        rank = bases.shape[2]
        rows = n * R
        vmem = pl.BlockSpec(memory_space=pltpu.VMEM)
        hbm = pl.BlockSpec(memory_space=pltpu.HBM)
        dma = pltpu.SemaphoreType.DMA

        def shape(a):
            return jax.ShapeDtypeStruct(a.shape, f32)

        W = key_weight.shape[1]
        outs = (
            shape(key_weight), shape(out_weight), shape(key_weight), shape(out_weight),
            shape(first_moment), shape(second_moment),
            jax.ShapeDtypeStruct((D, W), bf16), jax.ShapeDtypeStruct((W, D), bf16),
        )
        V = pltpu.VMEM
        o = max(n - 1, 1)
        scratch = [
            V((R, W), f32), V((W, R), f32), V(bases.shape, bf16), V((2, R, Q), f32), V((2, R, Q), f32),
            V((2, nz, T, rows), bf16), V((2, T, K), bf16), V((2, T, rank), bf16),
            V((2, nz, n, n, R, Q), f32), V((2, nz, n, n, R, Q), bf16), V((2, nz, n, n, R, Q), bf16),
            V((2, nz, n, n, R, Q), bf16), V((2, nz, o, n, R, Q), bf16),
            V((nz, n, R, Q), f32), V((nz, n, R, Q), bf16), V((nz, o, R, Q), bf16),
            V((nz - 1, R, Q), bf16), V((nz - 1, R, Q), bf16),
            V((n, R, Q), f32), V((nz - 1, n, R, Q), bf16), V((nz - 1, n, R, Q), bf16),
            V((n, R, Q), bf16), V((o, R, Q), bf16),
            V((2, tp, R, Q), bf16),
            V((2, 8, 128), f32), V((2, tp - 1, 8, 128), f32), V((2, 8, 128), f32), V((2, fs - 1, 8, 128), f32),
            dma((2,)), dma((4,)), dma((2, 3)), dma((2, nz)), dma((2, nz)), dma((2, nz)),
            dma((2, nz, o)), dma((2, nz, o)), dma((nz, o)), dma((nz, o)),
            dma((2, nz - 1)), dma((2, nz - 1)), dma((o,)), dma((o,)),
            dma((2, tp - 1)), dma((2, tp - 1)), dma((2, tp - 1)), dma((2, tp - 1)),
            dma((2, fs - 1)), dma((2, fs - 1)), dma((2, 2, nz - 1)), dma((2, 2, nz - 1)),
            dma((2, nz, o)), dma((2, nz, o)),
        ]
        results = pl.pallas_call(
            functools.partial(kernel, fs, tp),
            out_shape=outs,
            in_specs=[hbm] * 9,
            out_specs=[vmem] * 8,
            scratch_shapes=scratch,
            compiler_params=pltpu.CompilerParams(
                collective_id=0, has_side_effects=True, vmem_limit_bytes=54 * 1024 * 1024
            ),
        )(saved_input, key_cot, mixed_out, out_cot, key_weight, out_weight, bases, first_moment, second_moment)
        return pl.pallas_call(
            move_out,
            out_shape=outs,
            in_specs=[pl.BlockSpec(memory_space=pl.ANY)] * 8,
            out_specs=[hbm] * 8,
            scratch_shapes=[dma((8,))],
            compiler_params=pltpu.CompilerParams(vmem_limit_bytes=1024 * 1024),
        )(*results)

    rows_placed = P(("fs", "tp"), None)
    return jax.shard_map(
        body,
        mesh=mesh,
        in_specs=(rows_placed,) * 4
        + (P("fs", "tp"), P("tp", "fs"), P(), P(None, "fs", "tp"), P(None, "fs", "tp")),
        out_specs=(
            P("fs", "tp"), P("tp", "fs"), P("fs", "tp"), P("tp", "fs"),
            P(None, "fs", "tp"), P(None, "fs", "tp"), P(None, "tp"), P("tp", None),
        ),
        check_vma=False,
    )
```

```python
import functools

import jax
import jax.numpy as jnp
from jax import lax
from jax.experimental import pallas as pl
from jax.experimental.pallas import tpu as pltpu
from jax.sharding import PartitionSpec as P

MESH = pl.DeviceIdType.MESH
f32 = jnp.float32
bf16 = jnp.bfloat16
first_decay = 0.8
second_decay = 0.9
learn_rate = 0.01


def kernel(
    fs, tp,
    x0_hbm, c0_hbm, c1_hbm, x1_hbm,
    key_w_hbm, out_w_hbm, bases_hbm, first_hbm, second_hbm,
    key_new, out_new, key_step, out_step, first_new, second_new, key_copy, out_copy,
    key_w, out_w, bases, first_m, second_m, x_buf, c_buf, mapped, own, csnd, crcv, s2snd, s2rcv,
    y_own, y_snd, y_rcv, z0_snd, z0_rcv, z1_own, z1_snd, z1_rcv, x1_snd, x1_rcv,
    dirs, ss_snd, ss_rcv, tt_snd, tt_rcv,
    b_in, w_in, c_in, x_in, c_send, c_recv, s2_send, s2_recv, y_send, y_recv,
    z_send, z_recv, xx_send, xx_recv, d_send, d_recv, sst_send, sst_recv,
    ttt_send, ttt_recv, gz_send, gz_recv, gy_send, gy_recv,
):
    n = tp // 2
    nz = fs // n
    R, Q = first_m.shape[1], first_m.shape[2]
    W = key_w.shape[1]
    T = x_buf.shape[2]
    rank = bases.shape[2]
    half = rank // 2
    rows = n * R
    fi, ti = lax.axis_index("fs"), lax.axis_index("tp")
    core, xi = lax.rem(ti, 2), ti // 2
    zi, yi = fi // n, lax.rem(fi, n)

    def at_x(p):
        return (fi, p * 2 + core)

    def at_y(p):
        return (zi * n + p, ti)

    def at_z(p):
        return (p * n + yi, ti)

    def peer(me, d, size):
        return lax.rem(me + d, size)

    chunk = [peer(zi, 1 + i, nz) for i in range(nz)]
    tiles = 3 if T % 3 == 0 else 1
    tile = T // tiles
    loads = {}
    for m, (c_hbm, x_hbm) in ((1, (c1_hbm, x1_hbm)), (0, (c0_hbm, x0_hbm))):
        loads["b", m] = pltpu.make_async_copy(bases_hbm.at[m], bases.at[m], b_in.at[m])
        for k in range(tiles):
            at = pl.ds(k * tile, tile)
            loads["c", m, k] = pltpu.make_async_copy(c_hbm.at[at], c_buf.at[m, at], c_in.at[m, k])
        for i in range(nz):
            cols = pl.ds(pl.multiple_of(chunk[i] * rows, 128), rows)
            loads[m, i] = pltpu.make_async_copy(x_hbm.at[:, cols], x_buf.at[m, i], x_in.at[m, i])
    rest = (
        (first_hbm, first_m), (second_hbm, second_m), (key_w_hbm, key_w), (out_w_hbm, out_w)
    )
    for k, (source, target) in enumerate(rest):
        loads["w", k] = pltpu.make_async_copy(source, target, w_in.at[k])
    items = [(m, i) for m in (1, 0) for i in range(nz)]
    for copy in loads.values():
        copy.start()

    sends = []

    def remote(src, dst, send, recv, where):
        copy = pltpu.make_async_remote_copy(
            src_ref=src, dst_ref=dst, send_sem=send, recv_sem=recv,
            device_id=where, device_id_type=MESH,
        )
        copy.start()
        sends.append(copy)
        return copy

    barrier = pltpu.get_barrier_semaphore()
    for d in range(1, tp):
        pl.semaphore_signal(barrier, inc=1, device_id=(fi, peer(ti, d, tp)), device_id_type=MESH)
    for d in range(1, fs):
        pl.semaphore_signal(barrier, inc=1, device_id=(peer(fi, d, fs), ti), device_id_type=MESH)

    def map_tokens(m):
        loads["b", m].wait()
        for k in range(tiles):
            loads["c", m, k].wait()
            at = pl.ds(k * tile, tile)
            both = jnp.dot(c_buf[m, at, :], bases[m], preferred_element_type=f32)
            blocks = [both[:, t * Q:(t + 1) * Q] for t in range(tp)]
            pairs = [(blocks[2 * x], blocks[2 * x + 1]) for x in range(n)]
            kept = [jnp.where(core == 0, a, b) for a, b in pairs]
            sent = [jnp.where(core == 0, b, a) for a, b in pairs]
            mapped[m, at, :] = jnp.concatenate(kept + sent, axis=1).astype(bf16)

    def multiply(m, i):
        loads[m, i].wait()
        part = lax.dot_general(
            x_buf[m, i], mapped[m], (((0,), (0,)), ((), ())), preferred_element_type=f32
        )
        for x in range(n):
            for y in range(n):
                at = (x, y) if m == 0 else (y, x)
                block = part[y * R:(y + 1) * R]
                own[m, i, at[0], at[1]] = block[:, x * Q:(x + 1) * Q]
                csnd[m, i, at[0], at[1]] = block[:, half + x * Q:half + (x + 1) * Q].astype(bf16)

    flows = {}

    def second_stage(m, i):
        flows["c", m, i].wait_recv()
        total = own[m, i] + crcv[m, i].astype(f32)
        own[m, i] = total
        s2snd[m, i] = total.astype(bf16)
        for d in range(1, n):
            p = peer((xi, yi)[m], d, n)
            flows["s2", m, i, d] = remote(
                s2snd.at[m, i, p], s2rcv.at[m, i, d - 1],
                s2_send.at[m, i, d - 1], s2_recv.at[m, i, d - 1], (at_x, at_y)[m](p),
            )

    def third_stage(m, i):
        total = own[m, i, (xi, yi)[m]]
        for d in range(1, n):
            flows["s2", m, i, d].wait_recv()
            total = total + s2rcv[m, i, d - 1].astype(f32)
        if m == 1:
            if i == nz - 1:
                z1_own[...] = total
            else:
                z1_snd[i] = total.astype(bf16)
                flows["z", 1, i] = remote(
                    z1_snd.at[i], z1_rcv.at[i], z_send.at[1, i], z_recv.at[1, i], at_z(chunk[i])
                )
        else:
            y_own[i] = total
            y_snd[i] = total.astype(bf16)
            for d in range(1, n):
                p = peer(yi, d, n)
                flows["y", i, d] = remote(
                    y_snd.at[i, p], y_rcv.at[i, d - 1],
                    y_send.at[i, d - 1], y_recv.at[i, d - 1], at_y(p),
                )

    def fourth_stage(i):
        total = y_own[i, yi]
        for d in range(1, n):
            flows["y", i, d].wait_recv()
            total = total + y_rcv[i, d - 1].astype(f32)
        if i == nz - 1:
            return total
        z0_snd[i] = total.astype(bf16)
        flows["z", 0, i] = remote(
            z0_snd.at[i], z0_rcv.at[i], z_send.at[0, i], z_recv.at[0, i], at_z(chunk[i])
        )

    def sum_z1():
        total = z1_own[...]
        for i in range(nz - 1):
            flows["z", 1, i].wait_recv()
            total = total + z1_rcv[i].astype(f32)
        z1_own[...] = total
        x1_snd[...] = total.astype(bf16)
        for d in range(1, n):
            p = peer(xi, d, n)
            flows["x", d] = remote(
                x1_snd.at[p], x1_rcv.at[d - 1], xx_send.at[d - 1], xx_recv.at[d - 1], at_x(p)
            )

    def sum_x1():
        total = z1_own[xi]
        for d in range(1, n):
            flows["x", d].wait_recv()
            total = total + x1_rcv[d - 1].astype(f32)
        return total

    def sum_z0(total):
        for i in range(nz - 1):
            flows["z", 0, i].wait_recv()
            total = total + z0_rcv[i].astype(f32)
        return total

    def update(m, reduced):
        first = first_decay * first_m[m] + (1.0 - first_decay) * reduced
        second = second_decay * second_m[m] + (1.0 - second_decay) * reduced * reduced
        direction = first / jnp.sqrt(second)
        squares = jnp.broadcast_to(jnp.sum(direction * direction, keepdims=True), (8, 128))
        ss_snd[m] = squares
        dirs[m, ti] = direction.astype(bf16)
        for d in range(1, tp):
            where = (fi, peer(ti, d, tp))
            flows["ss", m, d] = remote(
                ss_snd.at[m], ss_rcv.at[m, d - 1], sst_send.at[m, d - 1], sst_recv.at[m, d - 1], where
            )
            flows["d", m, d] = remote(
                dirs.at[m, ti], dirs.at[m, ti], d_send.at[m, d - 1], d_recv.at[m, d - 1], where
            )
        first_new[m] = first
        second_new[m] = second

    def sum_tp(m):
        squares = ss_snd[m]
        for d in range(1, tp):
            flows["ss", m, d].wait_recv()
            squares = squares + ss_rcv[m, d - 1]
        tt_snd[m] = squares
        for d in range(1, fs):
            flows["tt", m, d] = remote(
                tt_snd.at[m], tt_rcv.at[m, d - 1], ttt_send.at[m, d - 1], ttt_recv.at[m, d - 1],
                (peer(fi, d, fs), ti),
            )

    def project(m):
        for d in range(1, tp):
            flows["d", m, d].wait_recv()
        whole = jnp.concatenate([dirs[m, t] for t in range(tp)], axis=1)
        base = bases[m, pl.ds(pl.multiple_of(ti * W, 128), W), :]
        left, right = ((whole, base), (base, whole))[m]
        (key_step, out_step)[m][...] = lax.dot_general(
            left, right, (((1,), (1,)), ((), ())), preferred_element_type=f32
        )

    def key_at(z, y):
        return key_copy.at[pl.ds(pl.multiple_of((z * n + y) * R, 128), R), :]

    def out_at(z, y):
        return out_copy.at[:, pl.ds(pl.multiple_of((z * n + y) * R, 128), R)]

    pieces = (key_at, out_at)

    def line_copy(m, up, hop):
        piece = pieces[m](zi - hop if up else zi + hop, yi)
        side = 0 if up else 1
        return pltpu.make_async_remote_copy(
            src_ref=piece, dst_ref=piece, send_sem=gz_send.at[m, side, hop], recv_sem=gz_recv.at[m, side, hop],
            device_id=at_z(zi + 1 if up else zi - 1), device_id_type=MESH,
        )

    def may_send(up, hop):
        if up:
            return (zi >= hop) & (zi < nz - 1)
        return (zi + hop < nz) & (zi > 0)

    def side_copies(m, z):
        piece = pieces[m](z, yi)
        return [
            pltpu.make_async_remote_copy(
                src_ref=piece, dst_ref=piece, send_sem=gy_send.at[m, z, d - 1], recv_sem=gy_recv.at[m, z, d - 1],
                device_id=at_y(peer(yi, d, n)), device_id_type=MESH,
            )
            for d in range(1, n)
        ]

    def start_line(m, up, hop):
        @pl.when(may_send(up, hop))
        def _():
            line_copy(m, up, hop).start()

    def finish(m):
        squares = tt_snd[m]
        for d in range(1, fs):
            flows["tt", m, d].wait_recv()
            squares = squares + tt_rcv[m, d - 1]
        scale = lax.rsqrt(squares / (fs * R * rank) + 1.0)[0:1, 0:1]
        step_ref, new_ref, weight = ((key_step, key_new, key_w), (out_step, out_new, out_w))[m]
        step = step_ref[...] * scale
        new = weight[...] - learn_rate * step
        pieces[m](zi, yi)[...] = new.astype(bf16)
        for up in (True, False):
            start_line(m, up, 0)
        for copy in side_copies(m, zi):
            copy.start()
        step_ref[...] = step
        new_ref[...] = new

    def relay(m, hop):
        for up in (True, False):
            @pl.when((zi >= hop) if up else (zi + hop < nz))
            def _():
                line_copy(m, up, hop - 1).wait_recv()
                if hop < nz - 1:
                    start_line(m, up, hop)
                for copy in side_copies(m, zi - hop if up else zi + hop):
                    copy.start()

    def close(m):
        for z in range(nz):
            for copy in side_copies(m, z):
                copy.wait_recv()
        for z in range(nz):
            for copy in side_copies(m, z):
                copy.wait_send()
        for hop in range(nz - 1):
            for up in (True, False):
                @pl.when(may_send(up, hop))
                def _():
                    line_copy(m, up, hop).wait_send()

    for k, (m, i) in enumerate(items):
        if i == 0:
            map_tokens(m)
        multiply(m, i)
        if k == 0:
            pl.semaphore_wait(barrier, tp + fs - 2)
        flows["c", m, i] = remote(
            csnd.at[m, i], crcv.at[m, i], c_send.at[m, i], c_recv.at[m, i],
            (fi, xi * 2 + 1 - core),
        )
        if k >= 1:
            second_stage(*items[k - 1])
        if k >= 3:
            third_stage(*items[k - 3])
    second_stage(0, nz - 1)
    for k in range(len(rest)):
        loads["w", k].wait()
    for k in range(len(items) - 3, len(items)):
        if items[k][0] == 1:
            third_stage(*items[k])
    waiting = [items[k][1] for k in range(len(items) - 3, len(items)) if items[k][0] == 0]
    third_stage(0, waiting[0])
    sum_z1()
    for i in waiting[1:]:
        third_stage(0, i)
    for i in range(nz - 2):
        fourth_stage(i)
    update(1, sum_x1())
    fourth_stage(nz - 2)
    total0 = fourth_stage(nz - 1)
    sum_tp(1)
    project(1)
    update(0, sum_z0(total0))
    finish(1)
    sum_tp(0)
    relay(1, 1)
    project(0)
    finish(0)
    for hop in range(2, nz):
        relay(1, hop)
        relay(0, hop - 1)
    relay(0, nz - 1)
    close(1)
    close(0)
    for copy in sends:
        copy.wait_send()


def move_out(*refs):
    count = len(refs) // 2
    copies = [
        pltpu.make_async_copy(refs[k], refs[count + k], refs[-1].at[k]) for k in range(count)
    ]
    for copy in copies:
        copy.start()
    for copy in copies:
        copy.wait()


def solution(mesh):
    fs, tp = mesh.shape["fs"], mesh.shape["tp"]
    n = tp // 2
    nz = fs // n

    def body(saved_input, key_cot, mixed_out, out_cot, key_weight, out_weight, bases, first_moment, second_moment):
        R, Q = first_moment.shape[1:]
        T, D = saved_input.shape
        K = key_cot.shape[1]
        rank = bases.shape[2]
        rows = n * R
        vmem = pl.BlockSpec(memory_space=pltpu.VMEM)
        hbm = pl.BlockSpec(memory_space=pltpu.HBM)
        dma = pltpu.SemaphoreType.DMA

        def shape(a):
            return jax.ShapeDtypeStruct(a.shape, f32)

        W = key_weight.shape[1]
        outs = (
            shape(key_weight), shape(out_weight), shape(key_weight), shape(out_weight),
            shape(first_moment), shape(second_moment),
            jax.ShapeDtypeStruct((D, W), bf16), jax.ShapeDtypeStruct((W, D), bf16),
        )
        V = pltpu.VMEM
        o = max(n - 1, 1)
        scratch = [
            V((R, W), f32), V((W, R), f32), V(bases.shape, bf16), V((2, R, Q), f32), V((2, R, Q), f32),
            V((2, nz, T, rows), bf16), V((2, T, K), bf16), V((2, T, rank), bf16),
            V((2, nz, n, n, R, Q), f32), V((2, nz, n, n, R, Q), bf16), V((2, nz, n, n, R, Q), bf16),
            V((2, nz, n, n, R, Q), bf16), V((2, nz, o, n, R, Q), bf16),
            V((nz, n, R, Q), f32), V((nz, n, R, Q), bf16), V((nz, o, R, Q), bf16),
            V((nz - 1, R, Q), bf16), V((nz - 1, R, Q), bf16),
            V((n, R, Q), f32), V((nz - 1, n, R, Q), bf16), V((nz - 1, n, R, Q), bf16),
            V((n, R, Q), bf16), V((o, R, Q), bf16),
            V((2, tp, R, Q), bf16),
            V((2, 8, 128), f32), V((2, tp - 1, 8, 128), f32), V((2, 8, 128), f32), V((2, fs - 1, 8, 128), f32),
            dma((2,)), dma((4,)), dma((2, 3)), dma((2, nz)), dma((2, nz)), dma((2, nz)),
            dma((2, nz, o)), dma((2, nz, o)), dma((nz, o)), dma((nz, o)),
            dma((2, nz - 1)), dma((2, nz - 1)), dma((o,)), dma((o,)),
            dma((2, tp - 1)), dma((2, tp - 1)), dma((2, tp - 1)), dma((2, tp - 1)),
            dma((2, fs - 1)), dma((2, fs - 1)), dma((2, 2, nz - 1)), dma((2, 2, nz - 1)),
            dma((2, nz, o)), dma((2, nz, o)),
        ]
        results = pl.pallas_call(
            functools.partial(kernel, fs, tp),
            out_shape=outs,
            in_specs=[hbm] * 9,
            out_specs=[vmem] * 8,
            scratch_shapes=scratch,
            compiler_params=pltpu.CompilerParams(
                collective_id=0, has_side_effects=True, vmem_limit_bytes=51 * 1024 * 1024
            ),
        )(saved_input, key_cot, mixed_out, out_cot, key_weight, out_weight, bases, first_moment, second_moment)
        return pl.pallas_call(
            move_out,
            out_shape=outs,
            in_specs=[pl.BlockSpec(memory_space=pl.ANY)] * 8,
            out_specs=[hbm] * 8,
            scratch_shapes=[dma((8,))],
            compiler_params=pltpu.CompilerParams(vmem_limit_bytes=1024 * 1024),
        )(*results)

    rows_placed = P(("fs", "tp"), None)
    return jax.shard_map(
        body,
        mesh=mesh,
        in_specs=(rows_placed,) * 4
        + (P("fs", "tp"), P("tp", "fs"), P(), P(None, "fs", "tp"), P(None, "fs", "tp")),
        out_specs=(
            P("fs", "tp"), P("tp", "fs"), P("fs", "tp"), P("tp", "fs"),
            P(None, "fs", "tp"), P(None, "fs", "tp"), P(None, "tp"), P("tp", None),
        ),
        check_vma=False,
    )
```

```python
import functools

import jax
import jax.numpy as jnp
from jax import lax
from jax.experimental import pallas as pl
from jax.experimental.pallas import tpu as pltpu
from jax.sharding import PartitionSpec as P

MESH = pl.DeviceIdType.MESH
f32 = jnp.float32
bf16 = jnp.bfloat16
first_decay = 0.8
second_decay = 0.9
learn_rate = 0.01


def kernel(
    fs, tp,
    x0_hbm, c0_hbm, c1_hbm, x1_hbm,
    key_w_hbm, out_w_hbm, bases_hbm, first_hbm, second_hbm,
    key_new, out_new, key_step, out_step, first_new, second_new, key_copy, out_copy,
    key_w, out_w, bases, first_m, second_m, x_buf, c_buf, mapped, own, csnd, crcv, s2snd, s2rcv,
    y_own, y_snd, y_rcv, z0_snd, z0_rcv, z1_own, z1_snd, z1_rcv, x1_snd, x1_rcv,
    dirs, ss_snd, ss_rcv, tt_snd, tt_rcv,
    b_in, w_in, c_in, x_in, c_send, c_recv, s2_send, s2_recv, y_send, y_recv,
    z_send, z_recv, xx_send, xx_recv, d_send, d_recv, sst_send, sst_recv,
    ttt_send, ttt_recv, gz_send, gz_recv, gy_send, gy_recv,
):
    n = tp // 2
    nz = fs // n
    R, Q = first_m.shape[1], first_m.shape[2]
    W = key_w.shape[1]
    T = x_buf.shape[2]
    rank = bases.shape[2]
    half = rank // 2
    rows = n * R
    fi, ti = lax.axis_index("fs"), lax.axis_index("tp")
    core, xi = lax.rem(ti, 2), ti // 2
    zi, yi = fi // n, lax.rem(fi, n)

    def at_x(p):
        return (fi, p * 2 + core)

    def at_y(p):
        return (zi * n + p, ti)

    def at_z(p):
        return (p * n + yi, ti)

    def peer(me, d, size):
        return lax.rem(me + d, size)

    chunk = [peer(zi, 1 + i, nz) for i in range(nz)]
    tiles = 3 if T % 3 == 0 else 1
    tile = T // tiles
    loads = {}
    for m, (c_hbm, x_hbm) in ((1, (c1_hbm, x1_hbm)), (0, (c0_hbm, x0_hbm))):
        loads["b", m] = pltpu.make_async_copy(bases_hbm.at[m], bases.at[m], b_in.at[m])
        for k in range(tiles):
            at = pl.ds(k * tile, tile)
            loads["c", m, k] = pltpu.make_async_copy(c_hbm.at[at], c_buf.at[m, at], c_in.at[m, k])
        for i in range(nz):
            cols = pl.ds(pl.multiple_of(chunk[i] * rows, 128), rows)
            loads[m, i] = pltpu.make_async_copy(x_hbm.at[:, cols], x_buf.at[m, i], x_in.at[m, i])
    rest = (
        (first_hbm, first_m), (second_hbm, second_m), (key_w_hbm, key_w), (out_w_hbm, out_w)
    )
    for k, (source, target) in enumerate(rest):
        loads["w", k] = pltpu.make_async_copy(source, target, w_in.at[k])
    items = [(m, i) for m in (1, 0) for i in range(nz)]
    for copy in loads.values():
        copy.start()

    sends = []

    def remote(src, dst, send, recv, where):
        copy = pltpu.make_async_remote_copy(
            src_ref=src, dst_ref=dst, send_sem=send, recv_sem=recv,
            device_id=where, device_id_type=MESH,
        )
        copy.start()
        sends.append(copy)
        return copy

    barrier = pltpu.get_barrier_semaphore()
    for d in range(1, tp):
        pl.semaphore_signal(barrier, inc=1, device_id=(fi, peer(ti, d, tp)), device_id_type=MESH)
    for d in range(1, fs):
        pl.semaphore_signal(barrier, inc=1, device_id=(peer(fi, d, fs), ti), device_id_type=MESH)

    def map_tokens(m):
        loads["b", m].wait()
        for k in range(tiles):
            loads["c", m, k].wait()
            at = pl.ds(k * tile, tile)
            both = jnp.dot(c_buf[m, at, :], bases[m], preferred_element_type=f32)
            blocks = [both[:, t * Q:(t + 1) * Q] for t in range(tp)]
            pairs = [(blocks[2 * x], blocks[2 * x + 1]) for x in range(n)]
            kept = [jnp.where(core == 0, a, b) for a, b in pairs]
            sent = [jnp.where(core == 0, b, a) for a, b in pairs]
            mapped[m, at, :] = jnp.concatenate(kept + sent, axis=1).astype(bf16)

    def multiply(m, i):
        loads[m, i].wait()
        part = lax.dot_general(
            x_buf[m, i], mapped[m], (((0,), (0,)), ((), ())), preferred_element_type=f32
        )
        for x in range(n):
            for y in range(n):
                at = (x, y) if m == 0 else (y, x)
                block = part[y * R:(y + 1) * R]
                own[m, i, at[0], at[1]] = block[:, x * Q:(x + 1) * Q]
                csnd[m, i, at[0], at[1]] = block[:, half + x * Q:half + (x + 1) * Q].astype(bf16)

    flows = {}

    def second_stage(m, i):
        flows["c", m, i].wait_recv()
        total = own[m, i] + crcv[m, i].astype(f32)
        own[m, i] = total
        s2snd[m, i] = total.astype(bf16)
        for d in range(1, n):
            p = peer((xi, yi)[m], d, n)
            flows["s2", m, i, d] = remote(
                s2snd.at[m, i, p], s2rcv.at[m, i, d - 1],
                s2_send.at[m, i, d - 1], s2_recv.at[m, i, d - 1], (at_x, at_y)[m](p),
            )

    def third_stage(m, i):
        total = own[m, i, (xi, yi)[m]]
        for d in range(1, n):
            flows["s2", m, i, d].wait_recv()
            total = total + s2rcv[m, i, d - 1].astype(f32)
        if m == 1:
            if i == nz - 1:
                z1_own[...] = total
            else:
                z1_snd[i] = total.astype(bf16)
                flows["z", 1, i] = remote(
                    z1_snd.at[i], z1_rcv.at[i], z_send.at[1, i], z_recv.at[1, i], at_z(chunk[i])
                )
        else:
            y_own[i] = total
            y_snd[i] = total.astype(bf16)
            for d in range(1, n):
                p = peer(yi, d, n)
                flows["y", i, d] = remote(
                    y_snd.at[i, p], y_rcv.at[i, d - 1],
                    y_send.at[i, d - 1], y_recv.at[i, d - 1], at_y(p),
                )

    def fourth_stage(i):
        total = y_own[i, yi]
        for d in range(1, n):
            flows["y", i, d].wait_recv()
            total = total + y_rcv[i, d - 1].astype(f32)
        if i == nz - 1:
            return total
        z0_snd[i] = total.astype(bf16)
        flows["z", 0, i] = remote(
            z0_snd.at[i], z0_rcv.at[i], z_send.at[0, i], z_recv.at[0, i], at_z(chunk[i])
        )

    def sum_z1():
        total = z1_own[...]
        for i in range(nz - 1):
            flows["z", 1, i].wait_recv()
            total = total + z1_rcv[i].astype(f32)
        z1_own[...] = total
        x1_snd[...] = total.astype(bf16)
        for d in range(1, n):
            p = peer(xi, d, n)
            flows["x", d] = remote(
                x1_snd.at[p], x1_rcv.at[d - 1], xx_send.at[d - 1], xx_recv.at[d - 1], at_x(p)
            )

    def sum_x1():
        total = z1_own[xi]
        for d in range(1, n):
            flows["x", d].wait_recv()
            total = total + x1_rcv[d - 1].astype(f32)
        return total

    def sum_z0(total):
        for i in range(nz - 1):
            flows["z", 0, i].wait_recv()
            total = total + z0_rcv[i].astype(f32)
        return total

    def update(m, reduced):
        first = first_decay * first_m[m] + (1.0 - first_decay) * reduced
        second = second_decay * second_m[m] + (1.0 - second_decay) * reduced * reduced
        direction = first / jnp.sqrt(second)
        squares = jnp.broadcast_to(jnp.sum(direction * direction, keepdims=True), (8, 128))
        ss_snd[m] = squares
        dirs[m, ti] = direction.astype(bf16)
        for d in range(1, tp):
            where = (fi, peer(ti, d, tp))
            flows["ss", m, d] = remote(
                ss_snd.at[m], ss_rcv.at[m, d - 1], sst_send.at[m, d - 1], sst_recv.at[m, d - 1], where
            )
            flows["d", m, d] = remote(
                dirs.at[m, ti], dirs.at[m, ti], d_send.at[m, d - 1], d_recv.at[m, d - 1], where
            )
        first_new[m] = first
        second_new[m] = second

    def sum_tp(m):
        squares = ss_snd[m]
        for d in range(1, tp):
            flows["ss", m, d].wait_recv()
            squares = squares + ss_rcv[m, d - 1]
        tt_snd[m] = squares
        for d in range(1, fs):
            flows["tt", m, d] = remote(
                tt_snd.at[m], tt_rcv.at[m, d - 1], ttt_send.at[m, d - 1], ttt_recv.at[m, d - 1],
                (peer(fi, d, fs), ti),
            )

    def project(m):
        for d in range(1, tp):
            flows["d", m, d].wait_recv()
        whole = jnp.concatenate([dirs[m, t] for t in range(tp)], axis=1)
        base = bases[m, pl.ds(pl.multiple_of(ti * W, 128), W), :]
        left, right = ((whole, base), (base, whole))[m]
        (key_step, out_step)[m][...] = lax.dot_general(
            left, right, (((1,), (1,)), ((), ())), preferred_element_type=f32
        )

    def key_at(z, y):
        return key_copy.at[pl.ds(pl.multiple_of((z * n + y) * R, 128), R), :]

    def out_at(z, y):
        return out_copy.at[:, pl.ds(pl.multiple_of((z * n + y) * R, 128), R)]

    pieces = (key_at, out_at)

    def line_copy(m, up, hop):
        piece = pieces[m](zi - hop if up else zi + hop, yi)
        side = 0 if up else 1
        return pltpu.make_async_remote_copy(
            src_ref=piece, dst_ref=piece, send_sem=gz_send.at[m, side, hop], recv_sem=gz_recv.at[m, side, hop],
            device_id=at_z(zi + 1 if up else zi - 1), device_id_type=MESH,
        )

    def may_send(up, hop):
        if up:
            return (zi >= hop) & (zi < nz - 1)
        return (zi + hop < nz) & (zi > 0)

    def side_copies(m, z):
        piece = pieces[m](z, yi)
        return [
            pltpu.make_async_remote_copy(
                src_ref=piece, dst_ref=piece, send_sem=gy_send.at[m, z, d - 1], recv_sem=gy_recv.at[m, z, d - 1],
                device_id=at_y(peer(yi, d, n)), device_id_type=MESH,
            )
            for d in range(1, n)
        ]

    def start_line(m, up, hop):
        @pl.when(may_send(up, hop))
        def _():
            line_copy(m, up, hop).start()

    def finish(m):
        squares = tt_snd[m]
        for d in range(1, fs):
            flows["tt", m, d].wait_recv()
            squares = squares + tt_rcv[m, d - 1]
        scale = lax.rsqrt(squares / (fs * R * rank) + 1.0)[0:1, 0:1]
        step_ref, new_ref, weight = ((key_step, key_new, key_w), (out_step, out_new, out_w))[m]
        step = step_ref[...] * scale
        new = weight[...] - learn_rate * step
        pieces[m](zi, yi)[...] = new.astype(bf16)
        for up in (True, False):
            start_line(m, up, 0)
        for copy in side_copies(m, zi):
            copy.start()
        step_ref[...] = step
        new_ref[...] = new

    def relay(m, hop):
        for up in (True, False):
            @pl.when((zi >= hop) if up else (zi + hop < nz))
            def _():
                line_copy(m, up, hop - 1).wait_recv()
                if hop < nz - 1:
                    start_line(m, up, hop)
                for copy in side_copies(m, zi - hop if up else zi + hop):
                    copy.start()

    def close(m):
        for z in range(nz):
            for copy in side_copies(m, z):
                copy.wait_recv()
        for z in range(nz):
            for copy in side_copies(m, z):
                copy.wait_send()
        for hop in range(nz - 1):
            for up in (True, False):
                @pl.when(may_send(up, hop))
                def _():
                    line_copy(m, up, hop).wait_send()

    for k, (m, i) in enumerate(items):
        if i == 0:
            map_tokens(m)
        multiply(m, i)
        if k == 0:
            pl.semaphore_wait(barrier, tp + fs - 2)
        flows["c", m, i] = remote(
            csnd.at[m, i], crcv.at[m, i], c_send.at[m, i], c_recv.at[m, i],
            (fi, xi * 2 + 1 - core),
        )
        if k >= 1:
            second_stage(*items[k - 1])
        if k >= 3:
            third_stage(*items[k - 3])
    second_stage(0, nz - 1)
    for k in range(len(rest)):
        loads["w", k].wait()
    for k in range(len(items) - 3, len(items)):
        if items[k][0] == 1:
            third_stage(*items[k])
    waiting = [items[k][1] for k in range(len(items) - 3, len(items)) if items[k][0] == 0]
    third_stage(0, waiting[0])
    sum_z1()
    for i in waiting[1:]:
        third_stage(0, i)
    for i in range(nz - 2):
        fourth_stage(i)
    update(1, sum_x1())
    fourth_stage(nz - 2)
    total0 = fourth_stage(nz - 1)
    sum_tp(1)
    project(1)
    update(0, sum_z0(total0))
    finish(1)
    sum_tp(0)
    relay(1, 1)
    project(0)
    finish(0)
    for hop in range(2, nz):
        relay(1, hop)
        relay(0, hop - 1)
    relay(0, nz - 1)
    close(1)
    close(0)
    for copy in sends:
        copy.wait_send()


def move_out(*refs):
    count = len(refs) // 2
    copies = [
        pltpu.make_async_copy(refs[k], refs[count + k], refs[-1].at[k]) for k in range(count)
    ]
    for copy in copies:
        copy.start()
    for copy in copies:
        copy.wait()


def solution(mesh):
    fs, tp = mesh.shape["fs"], mesh.shape["tp"]
    n = tp // 2
    nz = fs // n

    def body(saved_input, key_cot, mixed_out, out_cot, key_weight, out_weight, bases, first_moment, second_moment):
        R, Q = first_moment.shape[1:]
        T, D = saved_input.shape
        K = key_cot.shape[1]
        rank = bases.shape[2]
        rows = n * R
        vmem = pl.BlockSpec(memory_space=pltpu.VMEM)
        hbm = pl.BlockSpec(memory_space=pltpu.HBM)
        dma = pltpu.SemaphoreType.DMA

        def shape(a):
            return jax.ShapeDtypeStruct(a.shape, f32)

        W = key_weight.shape[1]
        outs = (
            shape(key_weight), shape(out_weight), shape(key_weight), shape(out_weight),
            shape(first_moment), shape(second_moment),
            jax.ShapeDtypeStruct((D, W), bf16), jax.ShapeDtypeStruct((W, D), bf16),
        )
        V = pltpu.VMEM
        o = max(n - 1, 1)
        scratch = [
            V((R, W), f32), V((W, R), f32), V(bases.shape, bf16), V((2, R, Q), f32), V((2, R, Q), f32),
            V((2, nz, T, rows), bf16), V((2, T, K), bf16), V((2, T, rank), bf16),
            V((2, nz, n, n, R, Q), f32), V((2, nz, n, n, R, Q), bf16), V((2, nz, n, n, R, Q), bf16),
            V((2, nz, n, n, R, Q), bf16), V((2, nz, o, n, R, Q), bf16),
            V((nz, n, R, Q), f32), V((nz, n, R, Q), bf16), V((nz, o, R, Q), bf16),
            V((nz - 1, R, Q), bf16), V((nz - 1, R, Q), bf16),
            V((n, R, Q), f32), V((nz - 1, n, R, Q), bf16), V((nz - 1, n, R, Q), bf16),
            V((n, R, Q), bf16), V((o, R, Q), bf16),
            V((2, tp, R, Q), bf16),
            V((2, 8, 128), f32), V((2, tp - 1, 8, 128), f32), V((2, 8, 128), f32), V((2, fs - 1, 8, 128), f32),
            dma((2,)), dma((4,)), dma((2, 3)), dma((2, nz)), dma((2, nz)), dma((2, nz)),
            dma((2, nz, o)), dma((2, nz, o)), dma((nz, o)), dma((nz, o)),
            dma((2, nz - 1)), dma((2, nz - 1)), dma((o,)), dma((o,)),
            dma((2, tp - 1)), dma((2, tp - 1)), dma((2, tp - 1)), dma((2, tp - 1)),
            dma((2, fs - 1)), dma((2, fs - 1)), dma((2, 2, nz - 1)), dma((2, 2, nz - 1)),
            dma((2, nz, o)), dma((2, nz, o)),
        ]
        results = pl.pallas_call(
            functools.partial(kernel, fs, tp),
            out_shape=outs,
            in_specs=[hbm] * 9,
            out_specs=[vmem] * 8,
            scratch_shapes=scratch,
            compiler_params=pltpu.CompilerParams(
                collective_id=0, has_side_effects=True, vmem_limit_bytes=(48 if Q >= 128 else 54) * 1024 * 1024
            ),
        )(saved_input, key_cot, mixed_out, out_cot, key_weight, out_weight, bases, first_moment, second_moment)
        return pl.pallas_call(
            move_out,
            out_shape=outs,
            in_specs=[pl.BlockSpec(memory_space=pl.ANY)] * 8,
            out_specs=[hbm] * 8,
            scratch_shapes=[dma((8,))],
            compiler_params=pltpu.CompilerParams(vmem_limit_bytes=1024 * 1024),
        )(*results)

    rows_placed = P(("fs", "tp"), None)
    return jax.shard_map(
        body,
        mesh=mesh,
        in_specs=(rows_placed,) * 4
        + (P("fs", "tp"), P("tp", "fs"), P(), P(None, "fs", "tp"), P(None, "fs", "tp")),
        out_specs=(
            P("fs", "tp"), P("tp", "fs"), P("fs", "tp"), P("tp", "fs"),
            P(None, "fs", "tp"), P(None, "fs", "tp"), P(None, "tp"), P("tp", None),
        ),
        check_vma=False,
    )
```
